32 devices in a mesh: kv: 8 (over z, y), tp: 4 (over x, core).
Axes of the slice: x: 2, y: 2, z: 4, core: 2. Of those that a mesh axis runs over, the one named last changes fastest.
Arguments:
- block_in: bfloat16 [64, 4096], P(None, ('kv', 'tp')), may hold values from -30 to 30
- before_gain: bfloat16 [4096], P('kv'), may hold values from 0.099609375 to 1.8984375
- before_gate: bfloat16 [4096, 11264], P('kv', 'tp'), may hold values from -0.09375 to 0.09375
- before_up: bfloat16 [4096, 11264], P('kv', 'tp'), may hold values from -0.09375 to 0.09375
- before_down: bfloat16 [11264, 4096], P('tp', 'kv'), may hold values from -0.0546875 to 0.0546875
- mix_gain: bfloat16 [4096], P('kv'), may hold values from 0.099609375 to 1.8984375
- input_gate: bfloat16 [4096, 8192], P('kv', 'tp'), may hold values from -0.09375 to 0.09375
- input_value: bfloat16 [4096, 8192], P('kv', 'tp'), may hold values from -0.09375 to 0.09375
- input_write: bfloat16 [4096, 2048], P('kv', 'tp'), may hold values from -0.09375 to 0.09375
- input_read: bfloat16 [4096, 2048], P('kv', 'tp'), may hold values from -0.09375 to 0.09375
- input_step: bfloat16 [4096, 128], P('kv', 'tp'), may hold values from -0.09375 to 0.09375
- step_bias: float32 [128], P('tp'), may hold values from -3 to 0
- decay_log: float32 [128], P('tp'), may hold values from -1 to 1.4
- skip_gain: float32 [128], P('tp'), may hold values from 0.5 to 2
- value_taps: bfloat16 [4, 8192], P(None, 'tp'), may hold values from -3 to 3
- write_taps: bfloat16 [4, 2048], P(None, 'tp'), may hold values from -3 to 3
- read_taps: bfloat16 [4, 2048], P(None, 'tp'), may hold values from -3 to 3
- value_window: bfloat16 [64, 3, 8192], P('kv', None, 'tp'), may hold values from -6 to 6
- write_window: bfloat16 [64, 3, 2048], P('kv', None, 'tp'), may hold values from -6 to 6
- read_window: bfloat16 [64, 3, 2048], P('kv', None, 'tp'), may hold values from -6 to 6
- scan_state: float32 [64, 128, 64, 128], P('kv', 'tp'), may hold values from -2 to 2
- group_gain: bfloat16 [8192], P('tp'), may hold values from 0.099609375 to 1.8984375
- mixer_out: bfloat16 [8192, 4096], P('tp', 'kv'), may hold values from -0.0625 to 0.0625
- after_gain: bfloat16 [4096], P('kv'), may hold values from 0.099609375 to 1.8984375
- after_gate: bfloat16 [4096, 11264], P('kv', 'tp'), may hold values from -0.09375 to 0.09375
- after_up: bfloat16 [4096, 11264], P('kv', 'tp'), may hold values from -0.09375 to 0.09375
- after_down: bfloat16 [11264, 4096], P('tp', 'kv'), may hold values from -0.0546875 to 0.0546875
Outputs:
- block_out: bfloat16 [64, 4096], P(None, ('kv', 'tp'))
- state_next: float32 [64, 128, 64, 128], P('kv', 'tp')
- value_next: bfloat16 [64, 3, 8192], P('kv', None, 'tp')
- write_next: bfloat16 [64, 3, 2048], P('kv', None, 'tp')
- read_next: bfloat16 [64, 3, 2048], P('kv', None, 'tp')
The draws below stay inside these ranges and needn't reach their ends.
All inputs are finite; a program needn't handle non-finite values.
Results may differ from the reference program's by a relative error of at most 0.0085.
Values may be sent and summed in bfloat16 or wider, within the bound.
No kernel may reach another device: no remote copies, remote signals or barrier semaphores. Data moves between devices by JAX's collectives and lax.ppermute only.
A program may use at most 128 MiB of HBM per device.

```python
import math
import jax
import jax.numpy as jnp
from jax import lax

D = 4096
FF = 11264
INNER = 8192
HEAD_DIM = 64
HEADS = 128
GROUPS = 16
STATE = 128
CONV = 4
BATCH = 64
N_KV = 8
N_TP = 4


def draw_block_in(key, part):
    base_key = jax.random.fold_in(key, 11)
    first_key, second_key = jax.random.split(base_key, 2)
    columns = jnp.arange(D, dtype=jnp.int32)
    column_block = D // (N_KV * N_TP)
    tp_place = (columns // column_block % N_TP).astype(jnp.float32)
    column_scale = jnp.exp(1.6 * columns.astype(jnp.float32) / D + 0.7 * tp_place / max(N_TP - 1, 1))
    row_scale = jnp.exp(jax.random.uniform(second_key, (BATCH, 1), jnp.float32, 0.0, 1.1))
    values = jnp.clip(jax.random.normal(first_key, (BATCH, D), jnp.float32), -4.0, 4.0)
    return (0.25 * values * row_scale * column_scale[None, :]).astype(jnp.bfloat16)


def shard_levels(own_key, extent, shards, low, largest):
    loudness = 1.0
    for position, parts in shards:
        heights = jax.random.uniform(jax.random.fold_in(jax.random.fold_in(own_key, 6), position), (parts,), jnp.float32, low / len(shards), largest / len(shards))
        loudness = loudness * jnp.repeat(jnp.exp(heights), extent[position] // parts).reshape((-1,) + (1,) * (len(extent) - 1 - position))
    return loudness


def centred(stream_key, extent, spread, reach, shards=(), kind=jnp.bfloat16):
    entries = spread * jax.random.normal(stream_key, extent, jnp.float32)
    if shards:
        entries = entries * shard_levels(stream_key, extent, shards, -0.22, 0.18)
    return jnp.clip(entries, -reach, reach).astype(kind)


def setup_inputs(seed: int = 0) -> dict:
    arg_keys = jax.random.split(jax.random.key(seed), 28)
    block_in = draw_block_in(jax.random.fold_in(arg_keys[27], 71), 0)
    before_gain = jnp.clip(1.0 + 0.18 * jax.random.normal(arg_keys[1], (D,), jnp.float32), 0.099609375, 1.8984375).astype(jnp.bfloat16)
    before_gate = centred(arg_keys[2], (D, FF), D ** -0.5, 0.09375, ((0, 8), (1, 4)))
    before_up = centred(arg_keys[3], (D, FF), D ** -0.5, 0.09375, ((0, 8), (1, 4)))
    before_down = centred(arg_keys[4], (FF, D), FF ** -0.5, 0.0546875, ((0, 4), (1, 8)))
    mix_gain = jnp.clip(1.0 + 0.18 * jax.random.normal(arg_keys[5], (D,), jnp.float32), 0.099609375, 1.8984375).astype(jnp.bfloat16)
    input_gate = centred(arg_keys[6], (D, INNER), D ** -0.5, 0.09375, ((0, 8), (1, 4)))
    input_value = centred(arg_keys[7], (D, INNER), D ** -0.5, 0.09375, ((0, 8), (1, 4)))
    input_write = centred(arg_keys[8], (D, GROUPS * STATE), D ** -0.5, 0.09375, ((0, 8), (1, 4)))
    input_read = centred(arg_keys[9], (D, GROUPS * STATE), D ** -0.5, 0.09375, ((0, 8), (1, 4)))
    input_step = centred(arg_keys[10], (D, HEADS), D ** -0.5, 0.09375, ((0, 8), (1, 4)))
    step_bias = jnp.clip(-3.0 + 3.0 * jax.random.uniform(arg_keys[11], (HEADS,), jnp.float32) ** shard_levels(arg_keys[11], (HEADS,), ((0, 4),), -0.2, 0.2), -3.0, 0.0)
    decay_log = jnp.clip(-1.0 + 2.4 * jax.random.uniform(arg_keys[12], (HEADS,), jnp.float32) ** shard_levels(arg_keys[12], (HEADS,), ((0, 4),), -0.2, 0.2), -1.0, 1.4)
    skip_gain = jnp.clip(jnp.exp(math.log(2.0) - 1.3862944 * jax.random.uniform(arg_keys[13], (HEADS,), jnp.float32) ** shard_levels(arg_keys[13], (HEADS,), ((0, 4),), -0.2, 0.2)), 0.5, 2.0)
    value_taps = centred(arg_keys[14], (CONV, INNER), CONV ** -0.5, 3.0, ((1, 4),))
    write_taps = centred(arg_keys[15], (CONV, GROUPS * STATE), CONV ** -0.5, 3.0, ((1, 4),))
    read_taps = centred(arg_keys[16], (CONV, GROUPS * STATE), CONV ** -0.5, 3.0, ((1, 4),))
    value_window = centred(arg_keys[17], (BATCH, CONV - 1, INNER), 1.0, 6.0, ((0, 8), (2, 4)))
    write_window = centred(arg_keys[18], (BATCH, CONV - 1, GROUPS * STATE), 1.0, 6.0, ((0, 8), (2, 4)))
    read_window = centred(arg_keys[19], (BATCH, CONV - 1, GROUPS * STATE), 1.0, 6.0, ((0, 8), (2, 4)))
    scan_state = centred(arg_keys[20], (BATCH, HEADS, HEAD_DIM, STATE), 0.3, 2.0, ((0, 8), (1, 4)), jnp.float32)
    group_gain = jnp.clip(1.0 + 0.18 * jax.random.normal(arg_keys[21], (INNER,), jnp.float32), 0.099609375, 1.8984375).astype(jnp.bfloat16)
    mixer_out = centred(arg_keys[22], (INNER, D), INNER ** -0.5, 0.0625, ((0, 4), (1, 8)))
    after_gain = jnp.clip(1.0 + 0.18 * jax.random.normal(arg_keys[23], (D,), jnp.float32), 0.099609375, 1.8984375).astype(jnp.bfloat16)
    after_gate = centred(arg_keys[24], (D, FF), D ** -0.5, 0.09375, ((0, 8), (1, 4)))
    after_up = centred(arg_keys[25], (D, FF), D ** -0.5, 0.09375, ((0, 8), (1, 4)))
    after_down = centred(arg_keys[26], (FF, D), FF ** -0.5, 0.0546875, ((0, 4), (1, 8)))
    return dict(block_in=block_in, before_gain=before_gain, before_gate=before_gate, before_up=before_up, before_down=before_down, mix_gain=mix_gain, input_gate=input_gate, input_value=input_value, input_write=input_write, input_read=input_read, input_step=input_step, step_bias=step_bias, decay_log=decay_log, skip_gain=skip_gain, value_taps=value_taps, write_taps=write_taps, read_taps=read_taps, value_window=value_window, write_window=write_window, read_window=read_window, scan_state=scan_state, group_gain=group_gain, mixer_out=mixer_out, after_gain=after_gain, after_gate=after_gate, after_up=after_up, after_down=after_down)


EPS = 1e-06

def half_channel(current, gain_vec, gate_weight, up_weight, down_weight):
    widened = current.astype(jnp.float32)
    row_scale = lax.rsqrt(lax.optimization_barrier(jnp.mean(widened * widened, axis=1, keepdims=True)) + EPS)
    lifted = (widened * gain_vec.astype(jnp.float32)).astype(jnp.bfloat16)
    gate_sum = jnp.dot(lifted, gate_weight, preferred_element_type=jnp.float32) * row_scale
    up_sum = jnp.dot(lifted, up_weight, preferred_element_type=jnp.float32) * row_scale
    hidden = (jax.nn.silu(gate_sum) * up_sum).astype(jnp.bfloat16)
    down_sum = jnp.dot(hidden, down_weight, preferred_element_type=jnp.float32)
    return (widened + 0.5 * down_sum).astype(jnp.bfloat16)

def short_conv(window_state, fresh, taps):
    window = jnp.concatenate([window_state, fresh[:, None, :]], axis=1)
    conv_sum = lax.optimization_barrier(jnp.sum(window.astype(jnp.float32) * taps.astype(jnp.float32)[None], axis=1))
    return (jax.nn.silu(conv_sum), window[:, 1:])

def spread_groups(vectors, heads):
    count = vectors.shape[0]
    groups = vectors.shape[1] // STATE
    shaped = vectors.reshape(count, groups, 1, STATE)
    return jnp.broadcast_to(shaped, (count, groups, heads // groups, STATE)).reshape(count, heads, STATE)

def state_update(gate_rows, value_conv, write_conv, read_conv, step_raw, step_bias, decay_log, skip_gain, scan_state):
    count = value_conv.shape[0]
    heads = step_bias.shape[0]
    step_size = jax.nn.softplus(step_raw + step_bias[None, :])
    decay = jnp.exp(-step_size * jnp.exp(decay_log)[None, :])
    value_heads = value_conv.reshape(count, heads, HEAD_DIM)
    write_heads = spread_groups(write_conv, heads)
    read_heads = spread_groups(read_conv, heads)
    state_next = decay[:, :, None, None] * scan_state + (step_size[:, :, None] * value_heads)[:, :, :, None] * write_heads[:, :, None, :]
    readout = lax.optimization_barrier(jnp.sum(state_next * read_heads[:, :, None, :], axis=3)) + skip_gain[None, :, None] * value_heads
    gated = readout.reshape(count, heads * HEAD_DIM) * jax.nn.silu(gate_rows.astype(jnp.float32))
    groups = write_conv.shape[1] // STATE
    grouped = gated.reshape(count, groups, heads * HEAD_DIM // groups)
    grouped = grouped * lax.rsqrt(lax.optimization_barrier(jnp.mean(grouped * grouped, axis=2, keepdims=True)) + EPS)
    return (grouped.reshape(count, heads * HEAD_DIM), state_next)

def reference(block_in, before_gain, before_gate, before_up, before_down, mix_gain, input_gate, input_value, input_write, input_read, input_step, step_bias, decay_log, skip_gain, value_taps, write_taps, read_taps, value_window, write_window, read_window, scan_state, group_gain, mixer_out, after_gain, after_gate, after_up, after_down):
    first_out = half_channel(block_in, before_gain, before_gate, before_up, before_down)
    widened = first_out.astype(jnp.float32)
    mix_scale = lax.rsqrt(lax.optimization_barrier(jnp.mean(widened * widened, axis=1, keepdims=True)) + EPS)
    lifted = (widened * mix_gain.astype(jnp.float32)).astype(jnp.bfloat16)
    gate_rows = (jnp.dot(lifted, input_gate, preferred_element_type=jnp.float32) * mix_scale).astype(jnp.bfloat16)
    value_fresh = (jnp.dot(lifted, input_value, preferred_element_type=jnp.float32) * mix_scale).astype(jnp.bfloat16)
    write_fresh = (jnp.dot(lifted, input_write, preferred_element_type=jnp.float32) * mix_scale).astype(jnp.bfloat16)
    read_fresh = (jnp.dot(lifted, input_read, preferred_element_type=jnp.float32) * mix_scale).astype(jnp.bfloat16)
    step_raw = jnp.dot(lifted, input_step, preferred_element_type=jnp.float32) * mix_scale
    value_conv, value_next = short_conv(value_window, value_fresh, value_taps)
    write_conv, write_next = short_conv(write_window, write_fresh, write_taps)
    read_conv, read_next = short_conv(read_window, read_fresh, read_taps)
    normed, state_next = state_update(gate_rows, value_conv, write_conv, read_conv, step_raw, step_bias, decay_log, skip_gain, scan_state)
    mixer_rows = (normed * group_gain.astype(jnp.float32)[None, :]).astype(jnp.bfloat16)
    middle = (widened + jnp.dot(mixer_rows, mixer_out, preferred_element_type=jnp.float32)).astype(jnp.bfloat16)
    block_out = half_channel(middle, after_gain, after_gate, after_up, after_down)
    return (block_out, state_next, value_next, write_next, read_next)
```

```python
import jax
import jax.numpy as jnp
from jax import lax
from jax.experimental import pallas as pl
from jax.experimental.pallas import tpu as pltpu
from jax.sharding import PartitionSpec as P

D = 4096
HEAD_DIM = 64
STATE = 128
LANES = 128


EPS = 1e-06


def exchange(blocks, axis):
    return lax.all_to_all(blocks, axis, 0, 0)


def spread(block, axis):
    if axis == "tp":
        return lax.all_gather(block, axis, axis=0)
    return exchange(jnp.broadcast_to(block[None], (lax.axis_size(axis),) + block.shape), axis)


def chunk_of(width):
    count = 1
    while width // count > 1536 and width % (LANES * (count + 1)) == 0:
        count += 1
    while count > 1 and width % (LANES * count):
        count -= 1
    return width // count


def front(gathered, gain_vec, weights, exact_weight=None):
    rows, depth = gathered.shape
    exact = 0 if exact_weight is None else exact_weight.shape[1]
    tail = LANES
    pieces, at = [], 0
    for index, weight in enumerate(weights):
        size = chunk_of(weight.shape[1])
        for start in range(0, weight.shape[1], size):
            pieces.append((index, start, size, at))
            at += size
    total = at + tail
    operands = [gathered, gain_vec.reshape(1, depth)]
    specs = [pl.BlockSpec(memory_space=pltpu.VMEM)] * 2
    if exact:
        spare = jnp.zeros((depth, LANES - 2 * exact), exact_weight.dtype)
        operands.append(jnp.concatenate([exact_weight, exact_weight, spare], axis=1))
        specs.append(pl.BlockSpec(memory_space=pltpu.VMEM))
    fixed = len(operands)

    def kernel(*refs):
        sources = refs[fixed : fixed + len(weights)]
        out_ref = refs[fixed + len(weights)]
        held = refs[fixed + len(weights) + 1 : -1]
        arrived = refs[-1]
        copies = []
        for number, (index, start, size, _) in enumerate(pieces):
            copy = pltpu.make_async_copy(
                sources[index].at[:, pl.ds(start, size)], held[number], arrived.at[number]
            )
            copy.start()
            copies.append(copy)
        widened = refs[0][...].astype(jnp.float32)
        lifted = (widened * refs[1][...].astype(jnp.float32)).astype(jnp.bfloat16)
        squares = jnp.sum(widened * widened, axis=1, keepdims=True)
        squares_high = squares.astype(jnp.bfloat16).astype(jnp.float32)
        lane = lax.broadcasted_iota(jnp.int32, (rows, tail), 1)
        ending = jnp.where(
            lane == 2 * exact,
            squares_high,
            jnp.where(lane == 2 * exact + 1, squares - squares_high, 0.0),
        )
        if exact:
            product = jnp.dot(lifted, refs[2][...], preferred_element_type=jnp.float32)
            high = product.astype(jnp.bfloat16).astype(jnp.float32)
            twice = jnp.where(lane < exact, high, product - high)
            ending = jnp.where(lane < 2 * exact, twice, ending)
        out_ref[:, pl.ds(total - tail, tail)] = ending.astype(jnp.bfloat16)
        for number, (_, _, size, place) in enumerate(pieces):
            copies[number].wait()
            product = jnp.dot(lifted, held[number][...], preferred_element_type=jnp.float32)
            out_ref[:, pl.ds(place, size)] = product.astype(jnp.bfloat16)

    read = sum(weight.size for weight in weights) * 2
    return pl.pallas_call(
        kernel,
        out_shape=jax.ShapeDtypeStruct((rows, total), jnp.bfloat16),
        in_specs=specs + [pl.BlockSpec(memory_space=pl.ANY)] * len(weights),
        out_specs=pl.BlockSpec(memory_space=pltpu.VMEM),
        scratch_shapes=[pltpu.VMEM((depth, size), jnp.bfloat16) for _, _, size, _ in pieces]
        + [pltpu.SemaphoreType.DMA((len(pieces),))],
        cost_estimate=pl.CostEstimate(
            flops=2 * rows * depth * total, bytes_accessed=read, transcendentals=0
        ),
        name="front",
    )(*operands, *weights)


def sum_over_rows_owner(sent, widths, exact):
    devices = lax.axis_size("kv")
    got = exchange(sent.reshape(devices, sent.shape[0] // devices, sent.shape[1]), "kv")
    sums = jnp.sum(got.astype(jnp.float32), axis=0)
    outs, at = [], 0
    for width in widths:
        outs.append(sums[:, at : at + width])
        at += width
    if exact:
        outs.append(sums[:, at : at + exact] + sums[:, at + exact : at + 2 * exact])
        at += 2 * exact
    outs.append(sums[:, at : at + 1] + sums[:, at + 1 : at + 2])
    return outs


def all_rows(rows):
    got = spread(rows, "kv")
    return got.reshape(got.shape[0] * got.shape[1], got.shape[2])


def tp_sum(partial):
    return jnp.sum(spread(partial.astype(jnp.bfloat16), "tp").astype(jnp.float32), axis=0)


def tp_column_sum(partial):
    devices = lax.axis_size("tp")
    rows, columns = partial.shape
    blocks = partial.astype(jnp.bfloat16).reshape(rows, devices, columns // devices)
    got = exchange(blocks.transpose(1, 0, 2), "tp")
    return jnp.sum(got.astype(jnp.float32), axis=0)


def own_columns(full):
    size = full.shape[1] // lax.axis_size("tp")
    return lax.dynamic_slice_in_dim(full, lax.axis_index("tp") * size, size, axis=1)


def half_channel_part(gathered, gain_vec, gate_weight, up_weight, down_weight):
    sent = front(gathered, gain_vec, (gate_weight, up_weight))
    widths = (gate_weight.shape[1], up_weight.shape[1])
    gate_sum, up_sum, totals = sum_over_rows_owner(sent, widths, 0)
    row_scale = lax.rsqrt(totals / D + EPS)
    hidden = (jax.nn.silu(gate_sum * row_scale) * (up_sum * row_scale)).astype(jnp.bfloat16)
    return jnp.dot(all_rows(hidden), down_weight, preferred_element_type=jnp.float32)


def short_conv(window_state, fresh, taps):
    window = jnp.concatenate([window_state, fresh[:, None, :]], axis=1)
    conv_sum = jnp.sum(window.astype(jnp.float32) * taps.astype(jnp.float32)[None], axis=1)
    return (jax.nn.silu(conv_sum), window[:, 1:])


def spread_groups(vectors, heads):
    count = vectors.shape[0]
    groups = vectors.shape[1] // STATE
    shaped = vectors.reshape(count, groups, 1, STATE)
    return jnp.broadcast_to(shaped, (count, groups, heads // groups, STATE)).reshape(
        count, heads, STATE
    )


def state_update(
    gate_rows,
    value_conv,
    write_conv,
    read_conv,
    step_raw,
    step_bias,
    decay_log,
    skip_gain,
    scan_state,
):
    count = value_conv.shape[0]
    heads = step_bias.shape[0]
    step_size = jax.nn.softplus(step_raw + step_bias[None, :])
    decay = jnp.exp(-step_size * jnp.exp(decay_log)[None, :])
    value_heads = value_conv.reshape(count, heads, HEAD_DIM)
    write_heads = spread_groups(write_conv, heads)
    read_heads = spread_groups(read_conv, heads)
    state_next = (
        decay[:, :, None, None] * scan_state
        + (step_size[:, :, None] * value_heads)[:, :, :, None] * write_heads[:, :, None, :]
    )
    readout = (
        jnp.sum(state_next * read_heads[:, :, None, :], axis=3)
        + skip_gain[None, :, None] * value_heads
    )
    gated = readout.reshape(count, heads * HEAD_DIM) * jax.nn.silu(gate_rows.astype(jnp.float32))
    groups = write_conv.shape[1] // STATE
    grouped = gated.reshape(count, groups, heads * HEAD_DIM // groups)
    grouped = grouped * lax.rsqrt(jnp.mean(grouped * grouped, axis=2, keepdims=True) + EPS)
    return (grouped.reshape(count, heads * HEAD_DIM), state_next)


def local(
    block_in,
    before_gain,
    before_gate,
    before_up,
    before_down,
    mix_gain,
    input_gate,
    input_value,
    input_write,
    input_read,
    input_step,
    step_bias,
    decay_log,
    skip_gain,
    value_taps,
    write_taps,
    read_taps,
    value_window,
    write_window,
    read_window,
    scan_state,
    group_gain,
    mixer_out,
    after_gain,
    after_gate,
    after_up,
    after_down,
):
    columns = lax.all_gather(block_in, "tp", axis=1, tiled=True)
    down_part = half_channel_part(columns, before_gain, before_gate, before_up, before_down)
    first_out = (columns.astype(jnp.float32) + 0.5 * tp_sum(down_part)).astype(jnp.bfloat16)
    mixed = (input_gate, input_value, input_write, input_read)
    sent = front(first_out, mix_gain, mixed, input_step)
    widths = tuple(weight.shape[1] for weight in mixed)
    gate_sum, value_sum, write_sum, read_sum, step_sum, totals = sum_over_rows_owner(
        sent, widths, input_step.shape[1]
    )
    mix_scale = lax.rsqrt(totals / D + EPS)
    gate_rows = (gate_sum * mix_scale).astype(jnp.bfloat16)
    value_fresh = (value_sum * mix_scale).astype(jnp.bfloat16)
    write_fresh = (write_sum * mix_scale).astype(jnp.bfloat16)
    read_fresh = (read_sum * mix_scale).astype(jnp.bfloat16)
    step_raw = step_sum * mix_scale
    value_conv, value_next = short_conv(value_window, value_fresh, value_taps)
    write_conv, write_next = short_conv(write_window, write_fresh, write_taps)
    read_conv, read_next = short_conv(read_window, read_fresh, read_taps)
    normed, state_next = state_update(
        gate_rows,
        value_conv,
        write_conv,
        read_conv,
        step_raw,
        step_bias,
        decay_log,
        skip_gain,
        scan_state,
    )
    mixer_rows = (normed * group_gain.astype(jnp.float32)[None, :]).astype(jnp.bfloat16)
    back_part = jnp.dot(all_rows(mixer_rows), mixer_out, preferred_element_type=jnp.float32)
    middle = (first_out.astype(jnp.float32) + tp_sum(back_part)).astype(jnp.bfloat16)
    down_part = half_channel_part(middle, after_gain, after_gate, after_up, after_down)
    returned = tp_column_sum(down_part)
    block_out = (own_columns(middle).astype(jnp.float32) + 0.5 * returned).astype(jnp.bfloat16)
    return (block_out, state_next, value_next, write_next, read_next)


def solution(mesh):
    placed = (
        P(None, ("kv", "tp")),
        P("kv"),
        P("kv", "tp"),
        P("kv", "tp"),
        P("tp", "kv"),
        P("kv"),
        P("kv", "tp"),
        P("kv", "tp"),
        P("kv", "tp"),
        P("kv", "tp"),
        P("kv", "tp"),
        P("tp"),
        P("tp"),
        P("tp"),
        P(None, "tp"),
        P(None, "tp"),
        P(None, "tp"),
        P("kv", None, "tp"),
        P("kv", None, "tp"),
        P("kv", None, "tp"),
        P("kv", "tp", None, None),
        P("tp"),
        P("tp", "kv"),
        P("kv"),
        P("kv", "tp"),
        P("kv", "tp"),
        P("tp", "kv"),
    )
    return jax.shard_map(
        local,
        mesh=mesh,
        in_specs=placed,
        out_specs=(
            P(None, ("kv", "tp")),
            P("kv", "tp", None, None),
            P("kv", None, "tp"),
            P("kv", None, "tp"),
            P("kv", None, "tp"),
        ),
        check_vma=False,
    )
```

```python
import jax
import jax.numpy as jnp
from jax import lax
from jax.experimental import pallas as pl
from jax.experimental.pallas import tpu as pltpu
from jax.sharding import PartitionSpec as P

D = 4096
HEAD_DIM = 64
STATE = 128
LANES = 128


EPS = 1e-06


def exchange(blocks, axis):
    return lax.all_to_all(blocks, axis, 0, 0)


def spread(block, axis):
    if axis == "tp":
        return lax.all_gather(block, axis, axis=0)
    return exchange(jnp.broadcast_to(block[None], (lax.axis_size(axis),) + block.shape), axis)


def chunk_of(width):
    lanes = width // LANES
    fits = [n for n in range(1, lanes + 1) if lanes % n == 0 and n * LANES <= 4096]
    return max(fits) * LANES if width % LANES == 0 else width


def front(gathered, gain_vec, weights, exact_weight=None):
    rows, depth = gathered.shape
    exact = 0 if exact_weight is None else exact_weight.shape[1]
    tail = LANES
    pieces, at = [], 0
    for index, weight in enumerate(weights):
        size = chunk_of(weight.shape[1])
        for start in range(0, weight.shape[1], size):
            pieces.append((index, start, size, at))
            at += size
    total = at + tail
    operands = [gathered, gain_vec]
    specs = [pl.BlockSpec(memory_space=pltpu.VMEM)] * 2
    if exact:
        spare = jnp.zeros((depth, LANES - 2 * exact), exact_weight.dtype)
        operands.append(jnp.concatenate([exact_weight, exact_weight, spare], axis=1))
        specs.append(pl.BlockSpec(memory_space=pltpu.VMEM))
    fixed = len(operands)

    def kernel(*refs):
        sources = refs[fixed : fixed + len(weights)]
        out_ref = refs[fixed + len(weights)]
        widened = refs[0][...].astype(jnp.float32)
        lifted = (widened * refs[1][...].astype(jnp.float32)[None, :]).astype(jnp.bfloat16)
        squares = jnp.sum(widened * widened, axis=1, keepdims=True)
        squares_high = squares.astype(jnp.bfloat16).astype(jnp.float32)
        lane = lax.broadcasted_iota(jnp.int32, (rows, tail), 1)
        ending = jnp.where(
            lane == 2 * exact,
            squares_high,
            jnp.where(lane == 2 * exact + 1, squares - squares_high, 0.0),
        )
        if exact:
            product = jnp.dot(lifted, refs[2][...], preferred_element_type=jnp.float32)
            high = product.astype(jnp.bfloat16).astype(jnp.float32)
            twice = jnp.where(lane < exact, high, product - high)
            ending = jnp.where(lane < 2 * exact, twice, ending)
        out_ref[:, pl.ds(total - tail, tail)] = ending.astype(jnp.bfloat16)
        for index, start, size, place in pieces:
            weight = sources[index][:, pl.ds(start, size)]
            product = jnp.dot(lifted, weight, preferred_element_type=jnp.float32)
            out_ref[:, pl.ds(place, size)] = product.astype(jnp.bfloat16)

    read = sum(weight.size for weight in weights) * 2
    return pl.pallas_call(
        kernel,
        out_shape=jax.ShapeDtypeStruct((rows, total), jnp.bfloat16),
        in_specs=specs + [pl.BlockSpec(memory_space=pltpu.VMEM)] * len(weights),
        out_specs=pl.BlockSpec(memory_space=pltpu.VMEM),
        compiler_params=pltpu.CompilerParams(vmem_limit_bytes=16 << 20),
        cost_estimate=pl.CostEstimate(
            flops=2 * rows * depth * total, bytes_accessed=read, transcendentals=0
        ),
        name="front",
    )(*operands, *weights)


def sum_over_rows_owner(sent, widths, exact):
    devices = lax.axis_size("kv")
    got = exchange(sent.reshape(devices, sent.shape[0] // devices, sent.shape[1]), "kv")
    sums = jnp.sum(got.astype(jnp.float32), axis=0)
    outs, at = [], 0
    for width in widths:
        outs.append(sums[:, at : at + width])
        at += width
    if exact:
        outs.append(sums[:, at : at + exact] + sums[:, at + exact : at + 2 * exact])
        at += 2 * exact
    outs.append(sums[:, at : at + 1] + sums[:, at + 1 : at + 2])
    return outs


def all_rows(rows):
    got = spread(rows, "kv")
    return got.reshape(got.shape[0] * got.shape[1], got.shape[2])


def tp_sum(partial):
    return jnp.sum(spread(partial.astype(jnp.bfloat16), "tp").astype(jnp.float32), axis=0)


def tp_column_sum(partial):
    devices = lax.axis_size("tp")
    rows, columns = partial.shape
    blocks = partial.astype(jnp.bfloat16).reshape(rows, devices, columns // devices)
    got = exchange(blocks.transpose(1, 0, 2), "tp")
    return jnp.sum(got.astype(jnp.float32), axis=0)


def own_columns(full):
    size = full.shape[1] // lax.axis_size("tp")
    return lax.dynamic_slice_in_dim(full, lax.axis_index("tp") * size, size, axis=1)


def half_channel_part(gathered, gain_vec, gate_weight, up_weight, down_weight):
    sent = front(gathered, gain_vec, (gate_weight, up_weight))
    widths = (gate_weight.shape[1], up_weight.shape[1])
    gate_sum, up_sum, totals = sum_over_rows_owner(sent, widths, 0)
    row_scale = lax.rsqrt(totals / D + EPS)
    hidden = (jax.nn.silu(gate_sum * row_scale) * (up_sum * row_scale)).astype(jnp.bfloat16)
    return jnp.dot(all_rows(hidden), down_weight, preferred_element_type=jnp.float32)


def short_conv(window_state, fresh, taps):
    window = jnp.concatenate([window_state, fresh[:, None, :]], axis=1)
    conv_sum = jnp.sum(window.astype(jnp.float32) * taps.astype(jnp.float32)[None], axis=1)
    return (jax.nn.silu(conv_sum), window[:, 1:])


def spread_groups(vectors, heads):
    count = vectors.shape[0]
    groups = vectors.shape[1] // STATE
    shaped = vectors.reshape(count, groups, 1, STATE)
    return jnp.broadcast_to(shaped, (count, groups, heads // groups, STATE)).reshape(
        count, heads, STATE
    )


def state_update(
    gate_rows,
    value_conv,
    write_conv,
    read_conv,
    step_raw,
    step_bias,
    decay_log,
    skip_gain,
    scan_state,
):
    count = value_conv.shape[0]
    heads = step_bias.shape[0]
    step_size = jax.nn.softplus(step_raw + step_bias[None, :])
    decay = jnp.exp(-step_size * jnp.exp(decay_log)[None, :])
    value_heads = value_conv.reshape(count, heads, HEAD_DIM)
    write_heads = spread_groups(write_conv, heads)
    read_heads = spread_groups(read_conv, heads)
    state_next = (
        decay[:, :, None, None] * scan_state
        + (step_size[:, :, None] * value_heads)[:, :, :, None] * write_heads[:, :, None, :]
    )
    readout = (
        jnp.sum(state_next * read_heads[:, :, None, :], axis=3)
        + skip_gain[None, :, None] * value_heads
    )
    gated = readout.reshape(count, heads * HEAD_DIM) * jax.nn.silu(gate_rows.astype(jnp.float32))
    groups = write_conv.shape[1] // STATE
    grouped = gated.reshape(count, groups, heads * HEAD_DIM // groups)
    grouped = grouped * lax.rsqrt(jnp.mean(grouped * grouped, axis=2, keepdims=True) + EPS)
    return (grouped.reshape(count, heads * HEAD_DIM), state_next)


def local(
    block_in,
    before_gain,
    before_gate,
    before_up,
    before_down,
    mix_gain,
    input_gate,
    input_value,
    input_write,
    input_read,
    input_step,
    step_bias,
    decay_log,
    skip_gain,
    value_taps,
    write_taps,
    read_taps,
    value_window,
    write_window,
    read_window,
    scan_state,
    group_gain,
    mixer_out,
    after_gain,
    after_gate,
    after_up,
    after_down,
):
    columns = lax.all_gather(block_in, "tp", axis=1, tiled=True)
    down_part = half_channel_part(columns, before_gain, before_gate, before_up, before_down)
    first_out = (columns.astype(jnp.float32) + 0.5 * tp_sum(down_part)).astype(jnp.bfloat16)
    mixed = (input_gate, input_value, input_write, input_read)
    sent = front(first_out, mix_gain, mixed, input_step)
    widths = tuple(weight.shape[1] for weight in mixed)
    gate_sum, value_sum, write_sum, read_sum, step_sum, totals = sum_over_rows_owner(
        sent, widths, input_step.shape[1]
    )
    mix_scale = lax.rsqrt(totals / D + EPS)
    gate_rows = (gate_sum * mix_scale).astype(jnp.bfloat16)
    value_fresh = (value_sum * mix_scale).astype(jnp.bfloat16)
    write_fresh = (write_sum * mix_scale).astype(jnp.bfloat16)
    read_fresh = (read_sum * mix_scale).astype(jnp.bfloat16)
    step_raw = step_sum * mix_scale
    value_conv, value_next = short_conv(value_window, value_fresh, value_taps)
    write_conv, write_next = short_conv(write_window, write_fresh, write_taps)
    read_conv, read_next = short_conv(read_window, read_fresh, read_taps)
    normed, state_next = state_update(
        gate_rows,
        value_conv,
        write_conv,
        read_conv,
        step_raw,
        step_bias,
        decay_log,
        skip_gain,
        scan_state,
    )
    mixer_rows = (normed * group_gain.astype(jnp.float32)[None, :]).astype(jnp.bfloat16)
    back_part = jnp.dot(all_rows(mixer_rows), mixer_out, preferred_element_type=jnp.float32)
    middle = (first_out.astype(jnp.float32) + tp_sum(back_part)).astype(jnp.bfloat16)
    down_part = half_channel_part(middle, after_gain, after_gate, after_up, after_down)
    returned = tp_column_sum(down_part)
    block_out = (own_columns(middle).astype(jnp.float32) + 0.5 * returned).astype(jnp.bfloat16)
    return (block_out, state_next, value_next, write_next, read_next)


def solution(mesh):
    placed = (
        P(None, ("kv", "tp")),
        P("kv"),
        P("kv", "tp"),
        P("kv", "tp"),
        P("tp", "kv"),
        P("kv"),
        P("kv", "tp"),
        P("kv", "tp"),
        P("kv", "tp"),
        P("kv", "tp"),
        P("kv", "tp"),
        P("tp"),
        P("tp"),
        P("tp"),
        P(None, "tp"),
        P(None, "tp"),
        P(None, "tp"),
        P("kv", None, "tp"),
        P("kv", None, "tp"),
        P("kv", None, "tp"),
        P("kv", "tp", None, None),
        P("tp"),
        P("tp", "kv"),
        P("kv"),
        P("kv", "tp"),
        P("kv", "tp"),
        P("tp", "kv"),
    )
    return jax.shard_map(
        local,
        mesh=mesh,
        in_specs=placed,
        out_specs=(
            P(None, ("kv", "tp")),
            P("kv", "tp", None, None),
            P("kv", None, "tp"),
            P("kv", None, "tp"),
            P("kv", None, "tp"),
        ),
        check_vma=False,
    )
```
